128 devices in a mesh: ep: 128 (over z, y, x, core).
Axes of the slice: x: 4, y: 4, z: 4, core: 2. Of those that a mesh axis runs over, the one named last changes fastest.
Arguments:
- tokens: bfloat16 [3072, 2048], P('ep'), may hold values from -6 to 6
- lengths: int32 [3072], P('ep'), may hold values from 2 to 1024
- latent_cache: bfloat16 [3072, 1024, 256], P('ep'), may hold values from -500 to 500
- rotary_cache: bfloat16 [3072, 1024, 32], P('ep'), may hold values from -6 to 6
- route_ids: int32 [3072, 6], P('ep'), may hold values from 0 to 127, all different within a row; in each aligned block of 24 rows (0 to 23, 24 to 47, ...) at most 3 rows name the same one
- route_scores: float32 [3072, 6], P('ep'), may hold values from 0.05 to 1
- attn_gain: bfloat16 [2048], replicated, may hold values from 0.099609375 to 1.8984375
- w_query_down: bfloat16 [2048, 256], replicated, may hold values from -0.125 to 0.125
- query_gain: bfloat16 [256], replicated, may hold values from 0.099609375 to 1.8984375
- w_query_nope: bfloat16 [256, 2048], replicated, may hold values from -0.375 to 0.375
- w_query_rope: bfloat16 [256, 1024], replicated, may hold values from -0.375 to 0.375
- w_key_absorb: bfloat16 [32, 64, 256], replicated, may hold values from -0.75 to 0.75
- latent_gain: bfloat16 [256], replicated, may hold values from 0.099609375 to 1.8984375
- w_latent_down: bfloat16 [2048, 256], replicated, may hold values from -0.125 to 0.125
- w_rotary_key: bfloat16 [2048, 32], replicated, may hold values from -0.125 to 0.125
- w_value_up: bfloat16 [32, 256, 64], replicated, may hold values from -0.375 to 0.375
- w_output: bfloat16 [2048, 2048], P(None, 'ep'), may hold values from -0.125 to 0.125
- ffn_gain: bfloat16 [2048], replicated, may hold values from 0.099609375 to 1.8984375
- expert_gate: bfloat16 [128, 2048, 512], P('ep'), may hold values from -0.125 to 0.125
- expert_up: bfloat16 [128, 2048, 512], P('ep'), may hold values from -0.125 to 0.125
- expert_down: bfloat16 [128, 512, 2048], P('ep'), may hold values from -0.25 to 0.25
- shared_gate: bfloat16 [2048, 256], replicated, may hold values from -0.125 to 0.125
- shared_up: bfloat16 [2048, 256], replicated, may hold values from -0.125 to 0.125
- shared_down: bfloat16 [256, 2048], replicated, may hold values from -0.375 to 0.375
Outputs:
- mixed: bfloat16 [3072, 2048], P('ep')
- latent_new: bfloat16 [3072, 256], P('ep')
- rotary_new: bfloat16 [3072, 32], P('ep')
The draws below stay inside these ranges and needn't reach their ends.
Inputs may be any that keep to these rules, and one draw needn't show every extreme that they name: `route_ids`: within the rows of one device no expert is named by more than 3 rows, a bound that some block reaches; each row names 6 different experts. `lengths`: cache positions at or past a sequence's length are not read.
All inputs are finite; a program needn't handle non-finite values.
Results may differ from the reference program's by a relative error of at most 0.025.
Values may be sent and summed in bfloat16 or wider, within the bound.
No kernel may reach another device: no remote copies, remote signals or barrier semaphores. Data moves between devices by JAX's collectives and lax.ppermute only.
A program may use at most 128 MiB of HBM per device.

```python
import math
import jax
import jax.numpy as jnp
import numpy as np
from jax import lax

D = 2048
HEADS = 32
NOPE = 64
ROPE = 32
VDIM = 64
QRANK = 256
LAT = 256
EH = 512
SH = 256
TOP = 6
B_DEV = 24
CACHE = 1024
SEQS = 3072
EXPERTS = 128
CAP = 3
N_EP = 128


def draw_latent_cache(key, part):
    base = jnp.clip(jax.random.normal(jax.random.fold_in(key, 11), (SEQS, CACHE, LAT), jnp.float32), -6.0, 6.0)
    return base.astype(jnp.bfloat16)


def place_ends(drawn, rng, least, top_value):
    longest = drawn.shape.index(max(drawn.shape))
    spots = []
    for shift in (0, 1):
        where = [jax.random.randint(jax.random.fold_in(rng, axis), (), 0, length) for axis, length in enumerate(drawn.shape)]
        where[longest] = (where[longest] + shift) % drawn.shape[longest]
        spots.append(tuple(where))
    return drawn.at[spots[0]].set(least).at[spots[1]].set(top_value)


def shard_levels(own_key, shape, split, low, top_value):
    loudness = 1.0
    for dim, shards_of in split:
        heights = jax.random.uniform(jax.random.fold_in(jax.random.fold_in(own_key, 6), dim), (shards_of,), jnp.float32, low / len(split), top_value / len(split))
        loudness = loudness * jnp.repeat(jnp.exp(heights), shape[dim] // shards_of).reshape((-1,) + (1,) * (len(shape) - 1 - dim))
    return loudness


def routed_block(rng, own, number, rows, amount, top, most, lean):
    ranking = jax.random.permutation(rng, amount)
    crowded, ordinary = load_shares(amount, rows * top, most, lean, True), load_shares(amount, rows * top, most, lean, False)
    places = jnp.arange(amount)

    def named(tallies, turn):
        used = int((tallies > 0).sum())
        fixed = max(1, used // 4)
        passed = fixed + (places - fixed + turn * (used - fixed)) % max(1, amount - fixed)
        return jnp.zeros((amount,), jnp.int32).at[ranking[jnp.where(places < fixed, places, passed)]].set(jnp.asarray(tallies, jnp.int32))

    tallies = jnp.where(number % 4 == 0, named(crowded, number // 4), named(ordinary, number - number // 4 - 1))
    mixed = jax.random.permutation(jax.random.fold_in(own, 3), amount)
    donor, sink = mixed[0:amount // 2 * 2:2], mixed[1:amount // 2 * 2:2]
    margin = jnp.minimum(tallies[donor] - 1, most - tallies[sink]) // 2
    margin = jnp.where((donor == ranking[0]) | (sink == ranking[0]) | (tallies[sink] == 0), 0, jnp.maximum(margin, 0))
    passed = jax.random.randint(jax.random.fold_in(own, 4), (amount // 2,), 0, 1 << 20) % (margin + 1)
    tallies = tallies.at[donor].add(-passed).at[sink].add(passed)
    items = jnp.searchsorted(jnp.cumsum(tallies), jnp.arange(rows * top), side="right").astype(jnp.int32)
    grid = items.reshape(top, rows).T
    grid = grid[jax.random.permutation(jax.random.fold_in(own, 1), rows)]
    turn = jax.random.randint(jax.random.fold_in(own, 2), (rows, 1), 0, top)
    return jnp.take_along_axis(grid, (jnp.arange(top)[None, :] + turn) % top, axis=1)


def load_shares(count, total, most, skew, full):
    loads = [(1 << 20) // math.isqrt(rank ** skew) + 1 for rank in range(1, count + 1)]
    largest = most if full else min(most, max(-(-total // count), total * loads[0] // sum(loads)))
    least = 1 if total - largest >= count - 1 else 0
    given, spare = [largest] + [least] * (count - 1), total - largest - least * (count - 1)
    while spare > 0:
        movable = [i for i in range(1, count) if given[i] < largest] or [i for i in range(1, count) if given[i] < most]
        mass, budget = sum([loads[i] for i in movable]), spare
        for i in movable:
            more = min(most - given[i], max(1, budget * loads[i] // mass), spare)
            given[i] = given[i] + more
            spare = spare - more
    return np.array(given)


def noise(own_key, extent, spread, limit, split=(), held_as=jnp.bfloat16):
    drawn = spread * jax.random.normal(own_key, extent, jnp.float32)
    if split:
        drawn = drawn * shard_levels(own_key, extent, split, -0.22, 0.18)
    return jnp.clip(drawn, -limit, limit).astype(held_as)


def setup_inputs(seed: int = 0) -> dict:
    keys = jax.random.split(jax.random.key(seed), 25)
    tokens = noise(keys[0], (SEQS, D), 1.0, 6.0, ((0, 128),))
    lengths = place_ends(jax.random.randint(keys[1], (SEQS,), 2, CACHE + 1), jax.random.fold_in(keys[1], 1), 2, CACHE).astype(jnp.int32)
    latent_cache = draw_latent_cache(jax.random.fold_in(keys[24], 71), 0)
    rotary_cache = noise(keys[3], (SEQS, CACHE, ROPE), 1.0, 6.0, ((0, 128),))
    route_ids_keys = jax.random.split(jax.random.fold_in(keys[4], 1), SEQS // B_DEV)
    route_ids_turns = jax.random.permutation(jax.random.fold_in(keys[4], 3), SEQS // B_DEV)
    route_ids = jax.vmap(lambda own, number: routed_block(jax.random.fold_in(keys[4], 2), own, number, B_DEV, EXPERTS, TOP, CAP, 2))(route_ids_keys, route_ids_turns).reshape((SEQS, TOP))
    route_scores = jnp.clip(0.05 + 0.95 * jax.random.uniform(keys[5], (SEQS, TOP), jnp.float32) ** shard_levels(keys[5], (SEQS, TOP), ((0, 128),), -0.2, 0.2), 0.05, 1.0)
    attn_gain = jnp.clip(1.0 + 0.18 * jax.random.normal(keys[6], (D,), jnp.float32), 0.099609375, 1.8984375).astype(jnp.bfloat16)
    w_query_down = noise(keys[7], (D, QRANK), D ** -0.5, 0.125)
    query_gain = jnp.clip(1.0 + 0.18 * jax.random.normal(keys[8], (QRANK,), jnp.float32), 0.099609375, 1.8984375).astype(jnp.bfloat16)
    w_query_nope = noise(keys[9], (QRANK, HEADS * NOPE), QRANK ** -0.5, 0.375)
    w_query_rope = noise(keys[10], (QRANK, HEADS * ROPE), QRANK ** -0.5, 0.375)
    w_key_absorb = noise(keys[11], (HEADS, NOPE, LAT), NOPE ** -0.5, 0.75)
    latent_gain = jnp.clip(1.0 + 0.18 * jax.random.normal(keys[12], (LAT,), jnp.float32), 0.099609375, 1.8984375).astype(jnp.bfloat16)
    w_latent_down = noise(keys[13], (D, LAT), D ** -0.5, 0.125)
    w_rotary_key = noise(keys[14], (D, ROPE), D ** -0.5, 0.125)
    w_value_up = noise(keys[15], (HEADS, LAT, VDIM), LAT ** -0.5, 0.375)
    w_output = noise(keys[16], (D, D), D ** -0.5, 0.125, ((1, 128),))
    ffn_gain = jnp.clip(1.0 + 0.18 * jax.random.normal(keys[17], (D,), jnp.float32), 0.099609375, 1.8984375).astype(jnp.bfloat16)
    expert_gate = noise(keys[18], (EXPERTS, D, EH), D ** -0.5, 0.125, ((0, 128),))
    expert_up = noise(keys[19], (EXPERTS, D, EH), D ** -0.5, 0.125, ((0, 128),))
    expert_down = noise(keys[20], (EXPERTS, EH, D), EH ** -0.5, 0.25, ((0, 128),))
    shared_gate = noise(keys[21], (D, SH), D ** -0.5, 0.125)
    shared_up = noise(keys[22], (D, SH), D ** -0.5, 0.125)
    shared_down = noise(keys[23], (SH, D), SH ** -0.5, 0.375)
    return dict(tokens=tokens, lengths=lengths, latent_cache=latent_cache, rotary_cache=rotary_cache, route_ids=route_ids, route_scores=route_scores, attn_gain=attn_gain, w_query_down=w_query_down, query_gain=query_gain, w_query_nope=w_query_nope, w_query_rope=w_query_rope, w_key_absorb=w_key_absorb, latent_gain=latent_gain, w_latent_down=w_latent_down, w_rotary_key=w_rotary_key, w_value_up=w_value_up, w_output=w_output, ffn_gain=ffn_gain, expert_gate=expert_gate, expert_up=expert_up, expert_down=expert_down, shared_gate=shared_gate, shared_up=shared_up, shared_down=shared_down)


EPSILON = 1e-06
THETA = 10000.0
ROUTED_SCALE = 2.5

def rms_scale(values, gain):
    squares = lax.optimization_barrier(jnp.mean(values * values, axis=-1, keepdims=True))
    return values * lax.rsqrt(squares + EPSILON) * gain.astype(jnp.float32)

def rotate(values, positions):
    half = values.shape[-1] // 2
    freqs = 1.0 / THETA ** (jnp.arange(half, dtype=jnp.float32) * 2.0 / values.shape[-1])
    angles = positions.astype(jnp.float32)[:, None] * freqs[None, :]
    if values.ndim == 3:
        angles = angles[:, None, :]
    cosine, sine = (jnp.cos(angles), jnp.sin(angles))
    first, second = (values[..., :half], values[..., half:])
    return jnp.concatenate([first * cosine - second * sine, second * cosine + first * sine], axis=-1)

def attend_block(tokens, lengths, latent_cache, rotary_cache, attn_gain, w_query_down, query_gain, w_query_nope, w_query_rope, w_key_absorb, latent_gain, w_latent_down, w_rotary_key, w_value_up):
    f32 = jnp.float32
    rows = tokens.shape[0]
    heads, nope, latent = w_key_absorb.shape
    rotary = w_rotary_key.shape[1]
    normed = rms_scale(tokens.astype(f32), attn_gain).astype(jnp.bfloat16)
    query_low = rms_scale(jnp.dot(normed, w_query_down, preferred_element_type=f32), query_gain).astype(jnp.bfloat16)
    query_nope = jnp.dot(query_low, w_query_nope, preferred_element_type=f32).astype(jnp.bfloat16).reshape(rows, heads, nope)
    query_rot = jnp.dot(query_low, w_query_rope, preferred_element_type=f32).reshape(rows, heads, rotary)
    query_rot = rotate(query_rot, lengths).astype(jnp.bfloat16)
    query_lat = jnp.einsum('thn,hnl->thl', query_nope.astype(f32), w_key_absorb.astype(f32)).astype(jnp.bfloat16)
    latent_new = rms_scale(jnp.dot(normed, w_latent_down, preferred_element_type=f32), latent_gain).astype(jnp.bfloat16)
    rotary_new = rotate(jnp.dot(normed, w_rotary_key, preferred_element_type=f32), lengths).astype(jnp.bfloat16)
    scale = (nope + rotary) ** (-0.5)
    scores = (jnp.einsum('thl,tkl->thk', query_lat.astype(f32), latent_cache.astype(f32)) + jnp.einsum('thr,tkr->thk', query_rot.astype(f32), rotary_cache.astype(f32))) * scale
    live = jnp.arange(latent_cache.shape[1], dtype=jnp.int32)[None, :] < lengths[:, None]
    scores = jnp.where(live[:, None, :], scores, -jnp.inf)
    own = (jnp.einsum('thl,tl->th', query_lat.astype(f32), latent_new.astype(f32)) + jnp.einsum('thr,tr->th', query_rot.astype(f32), rotary_new.astype(f32))) * scale
    top = jnp.maximum(lax.optimization_barrier(jnp.max(scores, axis=-1)), own)
    weights = jnp.exp(scores - top[..., None])
    own_weight = jnp.exp(own - top)
    total = lax.optimization_barrier(jnp.sum(weights, axis=-1)) + own_weight
    probs = (weights / total[..., None]).astype(jnp.bfloat16)
    own_prob = (own_weight / total).astype(jnp.bfloat16)
    out_lat = jnp.einsum('thk,tkl->thl', probs.astype(f32), latent_cache.astype(f32))
    out_lat = (out_lat + own_prob.astype(f32)[..., None] * latent_new.astype(f32)[:, None, :]).astype(jnp.bfloat16)
    values = jnp.einsum('thl,hlv->thv', out_lat.astype(f32), w_value_up.astype(f32)).astype(jnp.bfloat16)
    return (values.reshape(rows, heads * w_value_up.shape[2]), latent_new, rotary_new)

def reference(tokens, lengths, latent_cache, rotary_cache, route_ids, route_scores, attn_gain, w_query_down, query_gain, w_query_nope, w_query_rope, w_key_absorb, latent_gain, w_latent_down, w_rotary_key, w_value_up, w_output, ffn_gain, expert_gate, expert_up, expert_down, shared_gate, shared_up, shared_down):
    f32 = jnp.float32

    def one_block(pieces):
        return attend_block(pieces[0], pieces[1], pieces[2], pieces[3], attn_gain, w_query_down, query_gain, w_query_nope, w_query_rope, w_key_absorb, latent_gain, w_latent_down, w_rotary_key, w_value_up)
    values, latent_new, rotary_new = lax.map(one_block, (tokens.reshape(N_EP, B_DEV, D), lengths.reshape(N_EP, B_DEV), latent_cache.reshape(N_EP, B_DEV, CACHE, LAT), rotary_cache.reshape(N_EP, B_DEV, CACHE, ROPE)))
    values = values.reshape(SEQS, D)
    latent_new = latent_new.reshape(SEQS, LAT)
    rotary_new = rotary_new.reshape(SEQS, ROPE)
    attended = jnp.dot(values, w_output, preferred_element_type=f32).astype(jnp.bfloat16)
    residual = (tokens.astype(f32) + attended.astype(f32)).astype(jnp.bfloat16)
    ffn_in = rms_scale(residual.astype(f32), ffn_gain).astype(jnp.bfloat16)
    blocks = route_ids.reshape(N_EP, B_DEV * TOP)
    hits = (blocks[:, :, None] == jnp.arange(EXPERTS, dtype=jnp.int32)[None, None, :]).astype(jnp.int32)
    earlier = jnp.cumsum(hits, axis=1) - hits
    slot = lax.optimization_barrier(jnp.sum(earlier * hits, axis=2))
    global_slot = (jnp.arange(N_EP, dtype=jnp.int32)[:, None] * CAP + slot).reshape(-1)
    flat_ids = blocks.reshape(-1)
    pair_index = jnp.arange(SEQS * TOP, dtype=jnp.int32)
    table = jnp.full((EXPERTS, N_EP * CAP), SEQS * TOP, jnp.int32).at[flat_ids, global_slot].set(pair_index)
    padded = jnp.concatenate([jnp.repeat(ffn_in, TOP, axis=0), jnp.zeros((1, D), jnp.bfloat16)], axis=0)

    def one_expert(pieces):
        index, gate_w, up_w, down_w = pieces
        rows = padded[index]
        gate = jnp.dot(rows, gate_w, preferred_element_type=f32)
        upward = jnp.dot(rows, up_w, preferred_element_type=f32)
        hidden = (jax.nn.silu(gate) * upward).astype(jnp.bfloat16)
        return jnp.dot(hidden, down_w, preferred_element_type=f32).astype(jnp.bfloat16)
    outputs = lax.map(one_expert, (table, expert_gate, expert_up, expert_down))
    picked = outputs[flat_ids, global_slot].astype(f32).reshape(SEQS, TOP, D)
    route_weight = ROUTED_SCALE * route_scores / lax.optimization_barrier(jnp.sum(route_scores, axis=1, keepdims=True))
    routed = lax.optimization_barrier(jnp.sum(picked * route_weight[:, :, None], axis=1))
    gate_s = jnp.dot(ffn_in, shared_gate, preferred_element_type=f32)
    up_s = jnp.dot(ffn_in, shared_up, preferred_element_type=f32)
    hidden_s = (jax.nn.silu(gate_s) * up_s).astype(jnp.bfloat16)
    shared_out = jnp.dot(hidden_s, shared_down, preferred_element_type=f32)
    mixed = (residual.astype(f32) + routed + shared_out).astype(jnp.bfloat16)
    return (mixed, latent_new, rotary_new)
```

```python
import functools

import jax
import jax.numpy as jnp
from jax import lax
from jax.experimental import pallas as pl
from jax.experimental.pallas import tpu as pltpu
from jax.sharding import Mesh
from jax.sharding import PartitionSpec as P

EPSILON = 1e-06
THETA = 10000.0
ROUTED_SCALE = 2.5
f32 = jnp.float32
bf16 = jnp.bfloat16

NT = (((1,), (1,)), ((), ()))
NN = (((1,), (0,)), ((), ()))
SEQ_STEP = 4


def dot(a, b, dims=NN):
    return lax.dot_general(a, b, dims, preferred_element_type=f32)


def rms(values, gain):
    squares = jnp.mean(values * values, axis=-1, keepdims=True)
    return values * lax.rsqrt(squares + EPSILON) * gain


def turn(tile, cosine, sine):
    lane = lax.broadcasted_iota(jnp.int32, tile.shape, 1)
    swapped = jnp.where(lane % 32 < 16, pltpu.roll(tile, 112, 1), pltpu.roll(tile, 16, 1))
    return tile * cosine + swapped * sine


def attend_kernel(
    lengths,
    tokens,
    cosine,
    sine,
    latent,
    rotary,
    attn_gain,
    w_qd,
    q_gain,
    w_qn,
    w_qr,
    w_ka,
    l_gain,
    w_ld,
    w_rk,
    w_vu,
    values,
    latent_new,
    rotary_new,
    q_lat,
    q_rot,
    o_lat,
    l_new,
    r_new,
):
    step = pl.program_id(0)
    rows = tokens.shape[0]
    heads = w_ka.shape[0]
    lat = w_qd.shape[1]
    scale = (w_ka.shape[1] + w_rk.shape[0]) ** (-0.5)

    @pl.when(step == 0)
    def _():
        normed = rms(tokens[...].astype(f32), attn_gain[...].astype(f32)).astype(bf16)
        low = rms(dot(normed, w_qd[...]), q_gain[...].astype(f32)).astype(bf16)
        fresh = rms(dot(normed, w_ld[...]), l_gain[...].astype(f32)).astype(bf16)
        latent_new[...] = fresh
        l_new[...] = fresh.astype(f32)
        cos, sin = cosine[...], sine[...]
        w_four = jnp.concatenate([w_rk[...]] * 4, axis=0)
        turned = turn(dot(normed, w_four, NT), cos, sin).astype(bf16)
        rotary_new[...] = turned[:, :32]
        r_new[...] = turned.astype(f32)
        nope = dot(low, w_qn[...]).astype(bf16)
        for h in range(heads):
            part = dot(nope[:, h * 64 : h * 64 + 64], w_ka[h])
            for c in range(lat // 128):
                q_lat[c, pl.ds(h, rows, stride=heads), :] = part[:, c * 128 : c * 128 + 128]
        rope = dot(low, w_qr[...])
        for j in range(heads // 4):
            tile = turn(rope[:, j * 128 : j * 128 + 128], cos, sin)
            for q in range(4):
                shifted = tile if q == 0 else pltpu.roll(tile, 128 - 32 * q, 1)
                q_rot[pl.ds(4 * j + q, rows, stride=heads), :] = shifted

    cache = latent.shape[1]
    first = step * SEQ_STEP
    base = pl.multiple_of(first * heads, SEQ_STEP * heads)
    span = SEQ_STEP * heads
    q_all = jnp.concatenate(
        [q_lat[c, pl.ds(base, span), :] for c in range(lat // 128)], axis=1
    ).astype(bf16)
    owner = lax.broadcasted_iota(jnp.int32, (span, lat), 0) // heads
    group = lax.broadcasted_iota(jnp.int32, (heads, 128), 1) // 32
    lane = lax.broadcasted_iota(jnp.int32, (1, 128), 1) // 32
    rot_rows = []
    news = []
    new_rot = jnp.zeros((1, 128), f32)
    limit = jnp.zeros((1, 128), jnp.int32)
    scores = None
    own = None
    for j in range(SEQ_STEP):
        part = q_rot[pl.ds(base + j * heads, heads), :]
        part = part if j == 0 else pltpu.roll(part, 32 * j, 1)
        rot_rows.append(jnp.where(group == j, part, 0.0))
        new_rot = jnp.where(lane == j, r_new[pl.ds(first + j, 1), :], new_rot)
        limit = jnp.where(lane == j, lengths[first + j], limit)
        news.append(l_new[pl.ds(first + j, 1), :])
        q_j = jnp.where(owner == j, q_all, jnp.zeros_like(q_all))
        s_j = dot(latent[j], q_j, NT)
        o_j = dot(jnp.broadcast_to(news[j], (8, lat)).astype(bf16), q_j, NT)
        scores = s_j if j == 0 else scores + s_j
        own = o_j if j == 0 else own + o_j
    rot_q = jnp.concatenate(rot_rows, axis=0).astype(bf16)
    rot_keys = rotary[...].reshape(SEQ_STEP * 32, cache)
    scores = (scores + dot(rot_q, rot_keys).T) * scale
    own = (own + dot(jnp.broadcast_to(new_rot, (8, 128)).astype(bf16), rot_q, NT)) * scale
    own = own[:1]
    place = lax.broadcasted_iota(jnp.int32, scores.shape, 0)
    scores = jnp.where(place < limit, scores, -jnp.inf)
    top = jnp.maximum(jnp.max(scores, axis=0, keepdims=True), own)
    weights = jnp.exp(scores - top)
    own_weight = jnp.exp(own - top)
    inverse = 1.0 / (jnp.sum(weights, axis=0, keepdims=True) + own_weight)
    probs = (weights * inverse).T.astype(bf16)
    own_prob = jnp.broadcast_to((own_weight * inverse).astype(bf16).astype(f32), (8, 128)).T
    for j in range(SEQ_STEP):
        sl = slice(j * heads, (j + 1) * heads)
        out = dot(probs[sl], latent[j]) + own_prob[sl, :1] * news[j]
        for c in range(lat // 128):
            o_lat[c, pl.ds(base + j * heads, heads), :] = out[:, c * 128 : c * 128 + 128]

    @pl.when(step == pl.num_programs(0) - 1)
    def _():
        for g in range(heads // 2):
            pair = []
            for h in (2 * g, 2 * g + 1):
                rows_h = jnp.concatenate(
                    [o_lat[c, pl.ds(h, rows, stride=heads), :] for c in range(lat // 128)], axis=1
                ).astype(bf16)
                pair.append(dot(rows_h, w_vu[h], NT))
            values[:, g * 128 : g * 128 + 128] = jnp.concatenate(pair, axis=1).astype(bf16)


def whole(shape):
    zeros = (0,) * len(shape)
    return pl.BlockSpec(shape, lambda *_: zeros)


def smem():
    return pl.BlockSpec(memory_space=pltpu.SMEM)


def vmem():
    return pl.BlockSpec(memory_space=pltpu.VMEM)


def room(mib):
    return pltpu.CompilerParams(vmem_limit_bytes=mib * 2**20)


def near_core(*arrays):
    return [pltpu.with_memory_space_constraint(a, pltpu.VMEM) for a in arrays]


def attend(lengths, tokens, cosine, sine, latent, rotary, *weights):
    rows, model = tokens.shape
    cache, lat = latent.shape[1:]
    rope = rotary.shape[1]
    heads = weights[5].shape[0]
    return pl.pallas_call(
        attend_kernel,
        grid=(rows // SEQ_STEP,),
        in_specs=[
            smem(),
            whole(tokens.shape),
            whole(cosine.shape),
            whole(sine.shape),
            pl.BlockSpec((SEQ_STEP, cache, lat), lambda i: (i, 0, 0)),
            pl.BlockSpec((SEQ_STEP, rope, cache), lambda i: (i, 0, 0)),
            *[whole(w.shape) for w in weights],
        ],
        out_specs=[whole((rows, model)), whole((rows, lat)), whole((rows, rope))],
        out_shape=[
            jax.ShapeDtypeStruct((rows, model), bf16),
            jax.ShapeDtypeStruct((rows, lat), bf16),
            jax.ShapeDtypeStruct((rows, rope), bf16),
        ],
        scratch_shapes=[
            pltpu.VMEM((lat // 128, rows * heads, 128), f32),
            pltpu.VMEM((rows * heads, 128), f32),
            pltpu.VMEM((lat // 128, rows * heads, 128), f32),
            pltpu.VMEM((rows, lat), f32),
            pltpu.VMEM((rows, 128), f32),
        ],
        cost_estimate=pl.CostEstimate(
            flops=4 * 10**9, bytes_accessed=22 * 10**6, transcendentals=10**6
        ),
        compiler_params=room(32),
        name="attend",
    )(
        lengths,
        tokens,
        cosine,
        sine,
        *[pltpu.with_memory_space_constraint(a, pltpu.HBM) for a in (latent, rotary, *weights)],
    )


def project_kernel(side, mine, other, v0, v1, v2, out, w):
    c = side[0]
    w[:, c] = mine[...]
    w[:, 1 - c] = other[...]
    columns = w[...].reshape(w.shape[0] * 2 * w.shape[2], w.shape[3])
    vals = jnp.concatenate([v0[...], v1[...], v2[...]], axis=0)
    out[...] = dot(vals, columns, NT).astype(bf16)


def project(side, mine, other, v0, v1, v2):
    groups, cols, model = mine.shape
    rows = v0.shape[0] + v1.shape[0] + v2.shape[0]
    return pl.pallas_call(
        project_kernel,
        in_specs=[smem()] + [vmem()] * 5,
        out_specs=vmem(),
        out_shape=pltpu.VMEM((rows, groups * 2 * cols), bf16),
        scratch_shapes=[pltpu.VMEM((groups, 2, cols, model), bf16)],
        compiler_params=room(12),
        name="project",
    )(side, *near_core(mine, other, v0, v1, v2))


def dispatch_kernel(place, target, here, far, near, tokens, gain, out, residual, ffn, blocks, tiles):
    z = place[0]
    rows = tokens.shape[0]
    blocks[z] = here[:rows]
    blocks[3 - z] = far[:rows]
    blocks[z ^ 1] = near[0]
    blocks[(3 - z) ^ 1] = near[1]
    attended = jnp.concatenate([blocks[b] for b in range(4)], axis=1)
    total = (tokens[...].astype(f32) + attended.astype(f32)).astype(bf16)
    residual[...] = total
    normed = rms(total.astype(f32), gain[...].astype(f32))
    ffn[...] = normed.astype(bf16)
    for c in range(16):
        tiles[pl.ds(c, rows, stride=16), :] = normed[:, c * 128 : c * 128 + 128]
    out[...] = jnp.zeros_like(out)

    def send(t, _):
        tile = tiles[pl.ds(pl.multiple_of(t * 16, 16), 16), :].astype(bf16)
        for k in range(6):
            out[target[t * 6 + k]] = tile
        return _

    lax.fori_loop(0, rows, send, 0, unroll=4)


def dispatch(place, target, here, far, near, tokens, gain, slots):
    rows, model = tokens.shape
    return pl.pallas_call(
        dispatch_kernel,
        in_specs=[smem(), smem()] + [vmem()] * 5,
        out_specs=[vmem()] * 3,
        out_shape=[
            pltpu.VMEM((slots, 16, 128), bf16),
            pltpu.VMEM((rows, model), bf16),
            pltpu.VMEM((rows, model), bf16),
        ],
        scratch_shapes=[
            pltpu.VMEM((4, rows, model // 4), bf16),
            pltpu.VMEM((rows * 16, 128), f32),
        ],
        compiler_params=room(10),
        name="dispatch",
    )(place, target, *near_core(here, far, near, tokens, gain))


def shared_kernel(residual, ffn, gate, up, down, out):
    g = dot(ffn[...], gate[...])
    hidden = (g * jax.nn.sigmoid(g) * dot(ffn[...], up[...])).astype(bf16)
    out[...] = residual[...].astype(f32) + dot(hidden, down[...])


def shared(residual, ffn, gate, up, down):
    args = (residual, ffn, gate, up, down)
    return pl.pallas_call(
        shared_kernel,
        in_specs=[vmem()] * 5,
        out_specs=vmem(),
        out_shape=pltpu.VMEM(residual.shape, f32),
        cost_estimate=pl.CostEstimate(
            flops=10**9, bytes_accessed=4 * 10**6, transcendentals=10**4
        ),
        compiler_params=room(10),
        name="shared",
    )(*near_core(*args))


def expert_kernel(arrived, gate, up, down, out, wide, x):
    peers, depth, lanes = arrived.shape
    slots = depth // 16
    wide[...] = arrived[...].astype(f32).reshape(peers * depth, lanes)
    for s in range(slots):
        for c in range(16):
            rows = wide[pl.ds(s * 16 + c, peers, stride=depth), :]
            x[s * peers : (s + 1) * peers, c * 128 : c * 128 + 128] = rows.astype(bf16)
    g = dot(x[...], gate[0])
    hidden = (g * jax.nn.sigmoid(g) * dot(x[...], up[0])).astype(bf16)
    result = dot(hidden, down[0])
    for s in range(slots):
        for c in range(16):
            wide[pl.ds(s * 16 + c, peers, stride=depth), :] = result[
                s * peers : (s + 1) * peers, c * 128 : c * 128 + 128
            ]
    out[...] = wide[...].reshape(peers, depth, lanes).astype(bf16)


def experts(arrived, gate, up, down):
    peers, depth, lanes = arrived.shape
    return pl.pallas_call(
        expert_kernel,
        in_specs=[vmem()] * 4,
        out_specs=vmem(),
        out_shape=pltpu.VMEM(arrived.shape, bf16),
        scratch_shapes=[
            pltpu.VMEM((peers * depth, lanes), f32),
            pltpu.VMEM((peers * depth // 16, 2048), bf16),
        ],
        compiler_params=room(28),
        name="experts",
    )(*near_core(arrived, gate, up, down))


def combine_kernel(target, weight, returned, base, out, tiles):
    rows = base.shape[0]

    def gather(t, _):
        total = jnp.zeros((16, 128), f32)
        for k in range(6):
            p = t * 6 + k
            total = total + returned[target[p]].astype(f32) * weight[p]
        tiles[pl.ds(pl.multiple_of(t * 16, 16), 16), :] = total
        return _

    lax.fori_loop(0, rows, gather, 0, unroll=4)
    for c in range(16):
        sl = slice(c * 128, c * 128 + 128)
        out[:, sl] = (base[:, sl] + tiles[pl.ds(c, rows, stride=16), :]).astype(bf16)


def combine(target, weight, returned, base):
    rows = base.shape[0]
    return pl.pallas_call(
        combine_kernel,
        in_specs=[smem(), smem(), vmem(), vmem()],
        out_specs=vmem(),
        out_shape=pltpu.VMEM(base.shape, bf16),
        scratch_shapes=[pltpu.VMEM((rows * 16, 128), f32)],
        compiler_params=room(8),
        name="combine",
    )(target, weight, *near_core(returned, base))


def shards(
    tokens,
    lengths,
    latent_cache,
    rotary_cache,
    route_ids,
    route_scores,
    attn_gain,
    w_query_down,
    query_gain,
    w_query_nope,
    w_query_rope,
    w_key_absorb,
    latent_gain,
    w_latent_down,
    w_rotary_key,
    w_value_up,
    w_output,
    ffn_gain,
    expert_gate,
    expert_up,
    expert_down,
    shared_gate,
    shared_up,
    shared_down,
):
    rows, model = tokens.shape
    rotary = w_rotary_key.shape[1]
    top = route_ids.shape[1]
    devices = 128
    capacity = 3
    everyone = ("z", "y", "x", "c")
    z, c = lax.axis_index("z"), lax.axis_index("c")

    columns = w_output.T
    sent = jnp.broadcast_to(columns[None], (16,) + columns.shape)
    mine = lax.all_to_all(sent, ("y", "x"), 0, 0, tiled=True)

    half = rotary // 2
    freqs = 1.0 / THETA ** (jnp.arange(half, dtype=f32) * 2.0 / rotary)
    angles = lengths.astype(f32)[:, None] * jnp.tile(freqs, 8)[None, :]
    sign = jnp.where(jnp.arange(128) % rotary < half, -1.0, 1.0)
    cosine, sine = jnp.cos(angles), jnp.sin(angles) * sign[None, :]

    values, latent_new, rotary_new = attend(
        lengths,
        tokens,
        cosine,
        sine,
        latent_cache,
        rotary_cache.transpose(0, 2, 1),
        attn_gain[None],
        w_query_down,
        query_gain[None],
        w_query_nope,
        w_query_rope,
        w_key_absorb,
        latent_gain[None],
        w_latent_down,
        w_rotary_key.T,
        w_value_up.transpose(0, 2, 1),
    )

    same = route_ids[:, None, :, None] == route_ids[None, :, None, :]
    before = jnp.arange(rows)[None, :] < jnp.arange(rows)[:, None]
    slot = jnp.sum((same & before[:, :, None, None]).astype(jnp.int32), axis=(1, 3))
    target = (route_ids * capacity + slot).reshape(-1)
    weight = ROUTED_SCALE * route_scores / jnp.sum(route_scores, axis=1, keepdims=True)

    mine, values = lax.optimization_barrier((mine, values))
    other = lax.ppermute(mine, "c", [(0, 1), (1, 0)])
    pair = [(0, 1), (1, 0), (2, 3), (3, 2)]
    cross = [(0, 3), (3, 0), (1, 2), (2, 1)]
    v1 = lax.ppermute(values, "z", pair)
    both = jnp.concatenate([values, v1], axis=0)
    v2 = lax.ppermute(both, "z", cross)
    here = project(c.reshape(1), mine, other, values, v1, v2)
    far = lax.ppermute(here[2 * rows :], "z", cross)
    near = lax.ppermute(
        jnp.stack([here[rows : 2 * rows], far[rows:]], axis=0), "z", pair
    )
    out, residual, ffn = dispatch(
        z.reshape(1), target, here, far, near, tokens, ffn_gain[None], devices * capacity
    )
    arrived = lax.all_to_all(
        out.reshape(devices, capacity * 16, 128), everyone, 0, 0, tiled=True
    )
    base = shared(residual, ffn, shared_gate, shared_up, shared_down)
    result = experts(arrived, expert_gate, expert_up, expert_down)
    returned = lax.all_to_all(result, everyone, 0, 0, tiled=True)
    mixed = combine(
        target, weight.reshape(-1), returned.reshape(devices * capacity, 16, 128), base
    )
    return (mixed, latent_new, rotary_new)


def solution(mesh):
    grid = Mesh(mesh.devices.reshape(4, 4, 4, 2), ("z", "y", "x", "c"))
    ep = ("z", "y", "x", "c")
    return jax.shard_map(
        shards,
        mesh=grid,
        in_specs=(
            P(ep, None),
            P(ep),
            P(ep, None, None),
            P(ep, None, None),
            P(ep, None),
            P(ep, None),
            P(),
            P(),
            P(),
            P(),
            P(),
            P(),
            P(),
            P(),
            P(),
            P(),
            P(None, ep),
            P(),
            P(ep, None, None),
            P(ep, None, None),
            P(ep, None, None),
            P(),
            P(),
            P(),
        ),
        out_specs=(P(ep, None), P(ep, None), P(ep, None)),
        check_vma=False,
    )
```

```python
import functools

import jax
import jax.numpy as jnp
from jax import lax
from jax.experimental import pallas as pl
from jax.experimental.pallas import tpu as pltpu
from jax.sharding import Mesh
from jax.sharding import PartitionSpec as P

EPSILON = 1e-06
THETA = 10000.0
ROUTED_SCALE = 2.5
f32 = jnp.float32
bf16 = jnp.bfloat16

NT = (((1,), (1,)), ((), ()))
NN = (((1,), (0,)), ((), ()))
SEQ_STEP = 4


def dot(a, b, dims=NN):
    return lax.dot_general(a, b, dims, preferred_element_type=f32)


def rms(values, gain):
    squares = jnp.mean(values * values, axis=-1, keepdims=True)
    return values * lax.rsqrt(squares + EPSILON) * gain[None, :]


def turn(tile, cosine, sine):
    lane = lax.broadcasted_iota(jnp.int32, tile.shape, 1)
    swapped = jnp.where(lane % 32 < 16, pltpu.roll(tile, 112, 1), pltpu.roll(tile, 16, 1))
    return tile * cosine + swapped * sine


def attend_kernel(
    lengths,
    tokens,
    cosine,
    sine,
    attn_gain,
    q_gain,
    l_gain,
    w_qd_hbm,
    w_ld_hbm,
    w_rk_hbm,
    w_qn_hbm,
    w_ka_hbm,
    w_qr_hbm,
    w_vu_hbm,
    latent_hbm,
    rotary_hbm,
    values,
    latent_new,
    rotary_new,
    w_qd,
    w_ld,
    w_rk,
    w_qn,
    w_ka,
    w_qr,
    w_vu,
    latent,
    rotary,
    q_lat,
    q_rot,
    o_lat,
    l_new,
    r_new,
    scores_a,
    scores_b,
    sides_a,
    sides_b,
    sems,
):
    rows = tokens.shape[0]
    heads = w_ka.shape[0]
    lat = w_qd.shape[1]
    cache = latent.shape[1]
    halves = range(lat // 128)
    groups = rows // SEQ_STEP
    span = SEQ_STEP * heads
    rate = (w_ka.shape[1] + w_rk.shape[0]) ** (-0.5) * 1.4426950408889634
    moves = [
        pltpu.make_async_copy(a, b, sems.at[i])
        for i, (a, b) in enumerate(
            (
                (w_qd_hbm, w_qd),
                (w_ld_hbm, w_ld),
                (w_rk_hbm, w_rk),
                (w_qn_hbm, w_qn),
                (w_ka_hbm, w_ka),
                (w_qr_hbm, w_qr),
                (w_vu_hbm, w_vu),
            )
        )
    ]

    def fetches(g):
        part = pl.ds(g * SEQ_STEP, SEQ_STEP)
        return (
            pltpu.make_async_copy(latent_hbm.at[part], latent.at[part], sems.at[7 + g]),
            pltpu.make_async_copy(rotary_hbm.at[part], rotary.at[part], sems.at[7 + groups + g]),
        )

    for move in moves[:6]:
        move.start()
    for g in range(groups):
        for fetch in fetches(g):
            fetch.start()
    moves[6].start()

    normed = rms(tokens[...].astype(f32), attn_gain[...].astype(f32)).astype(bf16)
    moves[0].wait()
    low = rms(dot(normed, w_qd[...]), q_gain[...].astype(f32)).astype(bf16)
    moves[1].wait()
    fresh = rms(dot(normed, w_ld[...]), l_gain[...].astype(f32)).astype(bf16)
    latent_new[...] = fresh
    l_new[...] = fresh.astype(f32)
    cos, sin = cosine[...], sine[...]
    moves[2].wait()
    w_four = jnp.concatenate([w_rk[...]] * 4, axis=0)
    turned = turn(dot(normed, w_four, NT), cos, sin).astype(bf16)
    rotary_new[...] = turned[:, :32]
    r_new[...] = turned.astype(f32)
    moves[3].wait()
    nope = dot(low, w_qn[...]).astype(bf16)
    moves[4].wait()
    for h in range(heads):
        part = dot(nope[:, h * 64 : h * 64 + 64], w_ka[h])
        for g in range(rows // SEQ_STEP):
            at = g * span + h * SEQ_STEP
            for c in halves:
                q_lat[c, at : at + SEQ_STEP, :] = part[
                    g * SEQ_STEP : (g + 1) * SEQ_STEP, c * 128 : c * 128 + 128
                ]
    moves[5].wait()
    rope = dot(low, w_qr[...])
    member = lax.broadcasted_iota(jnp.int32, (rows, 128), 0) % SEQ_STEP
    inside = member == lax.broadcasted_iota(jnp.int32, (rows, 128), 1) // 32
    for j in range(heads // 4):
        tile = turn(rope[:, j * 128 : j * 128 + 128], cos, sin)
        moved = [tile] + [pltpu.roll(tile, 32 * k, 1) for k in (1, 2, 3)]
        for q in range(4):
            row = moved[-q % 4]
            for m in (1, 2, 3):
                row = jnp.where(member == m, moved[(m - q) % 4], row)
            row = jnp.where(inside, row, 0.0)
            for g in range(rows // SEQ_STEP):
                at = g * span + (4 * j + q) * SEQ_STEP
                q_rot[at : at + SEQ_STEP, :] = row[g * SEQ_STEP : (g + 1) * SEQ_STEP]

    owner = lax.broadcasted_iota(jnp.int32, (span, lat), 0) % SEQ_STEP
    group = lax.broadcasted_iota(jnp.int32, (1, 128), 1) // 32
    lane = lax.broadcasted_iota(jnp.int32, (1, span), 1) % SEQ_STEP
    place = lax.broadcasted_iota(jnp.int32, (cache, span), 0)
    mine = lax.broadcasted_iota(jnp.int32, (span, cache), 0) % SEQ_STEP

    def score(g, scores_ref, sides_ref):
        first = g * SEQ_STEP
        base = pl.multiple_of(g * span, span)
        for fetch in fetches(g):
            fetch.wait()
        q_all = jnp.concatenate([q_lat[c, pl.ds(base, span), :] for c in halves], axis=1).astype(
            bf16
        )
        new_rot = jnp.zeros((1, 128), f32)
        limit = jnp.zeros((1, span), jnp.int32)
        news, queries = [], []
        for j in range(SEQ_STEP):
            new_rot = jnp.where(group == j, r_new[pl.ds(first + j, 1), :], new_rot)
            limit = jnp.where(lane == j, lengths[first + j], limit)
            news.append(l_new[pl.ds(first + j, 1), :])
            queries.append(jnp.where(owner == j, q_all, jnp.zeros_like(q_all)))
        fresh = jnp.broadcast_to(jnp.concatenate(news, axis=1), (16, SEQ_STEP * lat)).astype(bf16)
        keys = jnp.concatenate([latent[first + j] for j in range(SEQ_STEP)], axis=1)
        rot_q = q_rot[pl.ds(base, span), :].astype(bf16)
        rot_keys = rotary[pl.ds(first, SEQ_STEP)].reshape(SEQ_STEP * 32, cache)
        turned = dot(rot_q, rot_keys).T
        both = dot(
            jnp.concatenate([keys, fresh], axis=0), jnp.concatenate(queries, axis=1), NT
        )
        own = dot(jnp.broadcast_to(new_rot, (16, 128)).astype(bf16), rot_q, NT)
        own = ((both[cache:] + own) * rate)[:1]
        scores = jnp.where(place < limit, (both[:cache] + turned) * rate, -jnp.inf)
        scores_ref[...] = scores
        top = jnp.maximum(jnp.max(scores, axis=0, keepdims=True), own)
        sides_ref[0:1, :] = top
        sides_ref[1:2, :] = jnp.exp2(own - top)

    def gather(g, scores_ref, sides_ref):
        first = g * SEQ_STEP
        base = pl.multiple_of(g * span, span)
        weights = jnp.exp2(scores_ref[...] - sides_ref[0:1, :])
        own_weight = sides_ref[1:2, :]
        inverse = 1.0 / (jnp.sum(weights, axis=0, keepdims=True) + own_weight)
        pick = lax.broadcasted_iota(jnp.int32, (8, span), 0) == 0
        sides = jnp.where(pick, inverse, own_weight).T
        probs = weights.T.astype(bf16)
        out = None
        for j in range(SEQ_STEP):
            part = dot(jnp.where(mine == j, probs, jnp.zeros_like(probs)), latent[first + j])
            out = part if j == 0 else out + part
        new_rows = l_new[pl.ds(first, 1), :]
        for j in range(1, SEQ_STEP):
            new_rows = jnp.where(owner == j, l_new[pl.ds(first + j, 1), :], new_rows)
        out = (out + sides[:, 1:2] * new_rows) * sides[:, :1]
        for c in halves:
            o_lat[c, pl.ds(base, span), :] = out[:, c * 128 : c * 128 + 128]

    score(0, scores_a, sides_a)

    def pair_of_groups(i, carry):
        g = 2 * i
        score(g + 1, scores_b, sides_b)
        gather(g, scores_a, sides_a)
        score(g + 2, scores_a, sides_a)
        gather(g + 1, scores_b, sides_b)
        return carry

    lax.fori_loop(0, groups // 2 - 1, pair_of_groups, 0)
    score(groups - 1, scores_b, sides_b)
    gather(groups - 2, scores_a, sides_a)
    gather(groups - 1, scores_b, sides_b)

    moves[6].wait()
    for p in range(heads // 2):
        pair = []
        for h in (2 * p, 2 * p + 1):
            parts = []
            for g in range(rows // SEQ_STEP):
                at = g * span + h * SEQ_STEP
                parts.append(
                    jnp.concatenate([o_lat[c, at : at + SEQ_STEP, :] for c in halves], axis=1)
                )
            pair.append(dot(jnp.concatenate(parts, axis=0).astype(bf16), w_vu[h], NT))
        values[:, p * 128 : p * 128 + 128] = jnp.concatenate(pair, axis=1).astype(bf16)


def whole(shape):
    zeros = (0,) * len(shape)
    return pl.BlockSpec(shape, lambda *_: zeros)


def smem():
    return pl.BlockSpec(memory_space=pltpu.SMEM)


def vmem():
    return pl.BlockSpec(memory_space=pltpu.VMEM)


def room(mib):
    return pltpu.CompilerParams(vmem_limit_bytes=mib * 2**20)


def far_away(array):
    return pltpu.with_memory_space_constraint(array, pltpu.HBM)


def near_core(*arrays):
    return [pltpu.with_memory_space_constraint(a, pltpu.VMEM) for a in arrays]


def attend(small, large):
    rows, model = small[1].shape
    lat, rope = large[0].shape[1], large[2].shape[0]
    heads = large[4].shape[0]
    far = pl.BlockSpec(memory_space=pl.ANY)
    groups = rows // SEQ_STEP
    return pl.pallas_call(
        attend_kernel,
        grid=(1,),
        in_specs=[smem()] + [whole(a.shape) for a in small[1:]] + [far] * len(large),
        out_specs=[vmem(), whole((rows, lat)), whole((rows, rope))],
        out_shape=[
            pltpu.VMEM((rows, model), bf16),
            jax.ShapeDtypeStruct((rows, lat), bf16),
            jax.ShapeDtypeStruct((rows, rope), bf16),
        ],
        scratch_shapes=[
            *[pltpu.VMEM(a.shape, bf16) for a in large],
            pltpu.VMEM((lat // 128, rows * heads, 128), f32),
            pltpu.VMEM((rows * heads, 128), f32),
            pltpu.VMEM((lat // 128, rows * heads, 128), f32),
            pltpu.VMEM((rows, lat), f32),
            pltpu.VMEM((rows, 128), f32),
            pltpu.VMEM((large[7].shape[1], SEQ_STEP * heads), f32),
            pltpu.VMEM((large[7].shape[1], SEQ_STEP * heads), f32),
            pltpu.VMEM((8, SEQ_STEP * heads), f32),
            pltpu.VMEM((8, SEQ_STEP * heads), f32),
            pltpu.SemaphoreType.DMA((7 + 2 * groups,)),
        ],
        cost_estimate=pl.CostEstimate(
            flops=4 * 10**9, bytes_accessed=22 * 10**6, transcendentals=10**6
        ),
        compiler_params=room(40),
        name="attend",
    )(*small, *[far_away(a) for a in large])


def copies_kernel(columns, out):
    for k in range(out.shape[0]):
        out[k] = columns[...]


def copies(columns, count):
    return pl.pallas_call(
        copies_kernel,
        in_specs=[vmem()],
        out_specs=vmem(),
        out_shape=pltpu.VMEM((count,) + columns.shape, bf16),
        compiler_params=room(4),
        name="copies",
    )(*near_core(columns))


def project_kernel(side, mine, other, v0, v1, v2, v3, o0, o1, o2, o3, w, sem):
    c = side[0]
    copy = pltpu.make_async_copy(other, w.at[:, 1 - c], sem.at[0])
    copy.start()
    copy_mine = pltpu.make_async_copy(mine, w.at[:, c], sem.at[1])
    copy_mine.start()
    rows = v0.shape[0]
    vals = jnp.concatenate([v0[...], v1[...], v2[...], v3[...]], axis=0)
    copy.wait()
    copy_mine.wait()
    columns = w[...].reshape(w.shape[0] * 2 * w.shape[2], w.shape[3])
    result = dot(vals, columns, NT).astype(bf16)
    for k, out in enumerate((o0, o1, o2, o3)):
        out[...] = result[k * rows : (k + 1) * rows]


def project(side, mine, other, *vals):
    groups, cols, model = mine.shape
    shape = (vals[0].shape[0], groups * 2 * cols)
    return pl.pallas_call(
        project_kernel,
        in_specs=[smem()] + [pl.BlockSpec(memory_space=pl.ANY)] * 2 + [vmem()] * 4,
        out_specs=[vmem()] * 4,
        out_shape=[pltpu.VMEM(shape, bf16)] * 4,
        scratch_shapes=[
            pltpu.VMEM((groups, 2, cols, model), bf16),
            pltpu.SemaphoreType.DMA((2,)),
        ],
        compiler_params=room(12),
        name="project",
    )(side, far_away(mine), far_away(other), *near_core(*vals))


def dispatch_kernel(
    place, target, h0, h1, h2, h3, tokens, gain, out, residual, ffn, blocks, tiles
):
    z = place[0]
    rows = tokens.shape[0]
    for k, block in enumerate((h0, h1, h2, h3)):
        blocks[(z + k) % 4] = block[...]
    attended = jnp.concatenate([blocks[b] for b in range(4)], axis=1)
    total = (tokens[...].astype(f32) + attended.astype(f32)).astype(bf16)
    residual[...] = total
    normed = rms(total.astype(f32), gain[...].astype(f32))
    ffn[...] = normed.astype(bf16)
    for c in range(16):
        tiles[pl.ds(c, rows, stride=16), :] = normed[:, c * 128 : c * 128 + 128]
    out[...] = jnp.zeros_like(out)

    def send(t, carry):
        tile = tiles[pl.ds(pl.multiple_of(t * 16, 16), 16), :].astype(bf16)
        for k in range(6):
            out[target[t * 6 + k]] = tile
        return carry

    lax.fori_loop(0, rows, send, 0, unroll=4)


def dispatch(place, target, h0, h1, h2, h3, tokens, gain, devices, capacity):
    rows, model = tokens.shape
    return pl.pallas_call(
        dispatch_kernel,
        in_specs=[smem(), smem()] + [vmem()] * 6,
        out_specs=[vmem()] * 3,
        out_shape=[
            pltpu.VMEM((devices * capacity, 16, 128), bf16),
            pltpu.VMEM((rows, model), bf16),
            pltpu.VMEM((rows, model), bf16),
        ],
        scratch_shapes=[
            pltpu.VMEM((4, rows, model // 4), bf16),
            pltpu.VMEM((rows * 16, 128), f32),
        ],
        compiler_params=room(10),
        name="dispatch",
    )(place, target, *near_core(h0, h1, h2, h3, tokens, gain))


def shared_kernel(residual, ffn, gate, up, down, out):
    g = dot(ffn[...], gate[...])
    hidden = (g * jax.nn.sigmoid(g) * dot(ffn[...], up[...])).astype(bf16)
    out[...] = residual[...].astype(f32) + dot(hidden, down[...])


def shared(residual, ffn, gate, up, down):
    args = (residual, ffn, gate, up, down)
    return pl.pallas_call(
        shared_kernel,
        in_specs=[vmem()] * 5,
        out_specs=vmem(),
        out_shape=pltpu.VMEM(residual.shape, f32),
        cost_estimate=pl.CostEstimate(
            flops=10**9, bytes_accessed=4 * 10**6, transcendentals=10**4
        ),
        compiler_params=room(10),
        name="shared",
    )(*near_core(*args))


def expert_kernel(arrived, gate, up, down, out, wide, x, w_down, sem):
    peers, depth, lanes = arrived.shape
    slots = depth // 16
    copy = pltpu.make_async_copy(down.at[0], w_down, sem)
    copy.start()
    wide[...] = arrived[...].astype(f32).reshape(peers * depth, lanes)
    for s in range(slots):
        for c in range(16):
            rows = wide[pl.ds(s * 16 + c, peers, stride=depth), :]
            x[s * peers : (s + 1) * peers, c * 128 : c * 128 + 128] = rows.astype(bf16)
    g = dot(x[...], gate[0])
    hidden = (g * jax.nn.sigmoid(g) * dot(x[...], up[0])).astype(bf16)
    copy.wait()
    result = dot(hidden, w_down[...])
    for s in range(slots):
        for c in range(16):
            wide[pl.ds(s * 16 + c, peers, stride=depth), :] = result[
                s * peers : (s + 1) * peers, c * 128 : c * 128 + 128
            ]
    out[...] = wide[...].reshape(peers, depth, lanes).astype(bf16)


def experts(arrived, gate, up, down):
    peers, depth, lanes = arrived.shape
    return pl.pallas_call(
        expert_kernel,
        in_specs=[vmem()] * 3 + [pl.BlockSpec(memory_space=pl.ANY)],
        out_specs=vmem(),
        out_shape=pltpu.VMEM(arrived.shape, bf16),
        scratch_shapes=[
            pltpu.VMEM((peers * depth, lanes), f32),
            pltpu.VMEM((peers * depth // 16, 2048), bf16),
            pltpu.VMEM(down.shape[1:], bf16),
            pltpu.SemaphoreType.DMA(()),
        ],
        compiler_params=room(20),
        name="experts",
    )(*near_core(arrived, gate, up), far_away(down))


def combine_kernel(target, weight, returned, base, out, tiles):
    rows = base.shape[0]

    def gather(t, carry):
        total = jnp.zeros((16, 128), f32)
        for k in range(6):
            p = t * 6 + k
            total = total + returned[target[p]].astype(f32) * weight[p]
        tiles[pl.ds(pl.multiple_of(t * 16, 16), 16), :] = total
        return carry

    lax.fori_loop(0, rows, gather, 0, unroll=4)
    for c in range(16):
        sl = slice(c * 128, c * 128 + 128)
        out[:, sl] = (base[:, sl] + tiles[pl.ds(c, rows, stride=16), :]).astype(bf16)


def combine(target, weight, returned, base):
    rows = base.shape[0]
    return pl.pallas_call(
        combine_kernel,
        in_specs=[smem(), smem(), vmem(), vmem()],
        out_specs=vmem(),
        out_shape=pltpu.VMEM(base.shape, bf16),
        scratch_shapes=[pltpu.VMEM((rows * 16, 128), f32)],
        compiler_params=room(8),
        name="combine",
    )(target, weight, *near_core(returned, base))


def shards(
    tokens,
    lengths,
    latent_cache,
    rotary_cache,
    route_ids,
    route_scores,
    attn_gain,
    w_query_down,
    query_gain,
    w_query_nope,
    w_query_rope,
    w_key_absorb,
    latent_gain,
    w_latent_down,
    w_rotary_key,
    w_value_up,
    w_output,
    ffn_gain,
    expert_gate,
    expert_up,
    expert_down,
    shared_gate,
    shared_up,
    shared_down,
):
    rows, model = tokens.shape
    rotary = w_rotary_key.shape[1]
    top = route_ids.shape[1]
    devices = 128
    capacity = 3
    everyone = ("z", "y", "x", "c")
    z, c = lax.axis_index("z"), lax.axis_index("c")

    columns = w_output.T
    sent = copies(columns, 16)
    mine = lax.all_to_all(sent, ("y", "x"), 0, 0, tiled=True)

    half = rotary // 2
    freqs = 1.0 / THETA ** (jnp.arange(half, dtype=f32) * 2.0 / rotary)
    angles = lengths.astype(f32)[:, None] * jnp.tile(freqs, 8)[None, :]
    sign = jnp.where(jnp.arange(128) % rotary < half, -1.0, 1.0)
    cosine, sine = jnp.cos(angles), jnp.sin(angles) * sign[None, :]

    values, latent_new, rotary_new = attend(
        (lengths, tokens, cosine, sine, attn_gain, query_gain, latent_gain),
        (
            w_query_down,
            w_latent_down,
            w_rotary_key.T,
            w_query_nope,
            w_key_absorb,
            w_query_rope,
            w_value_up.transpose(0, 2, 1),
            latent_cache,
            rotary_cache.transpose(0, 2, 1),
        ),
    )

    same = route_ids[:, None, :, None] == route_ids[None, :, None, :]
    before = jnp.arange(rows)[None, :] < jnp.arange(rows)[:, None]
    slot = jnp.sum((same & before[:, :, None, None]).astype(jnp.int32), axis=(1, 3))
    target = (route_ids * capacity + slot).reshape(-1)
    weight = ROUTED_SCALE * route_scores / jnp.sum(route_scores, axis=1, keepdims=True)

    mine, values = lax.optimization_barrier((mine, values))
    other = lax.ppermute(mine, "c", [(0, 1), (1, 0)])
    def shift(k):
        return [(i, (i + k) % 4) for i in range(4)]

    vals = [values] + [lax.ppermute(values, "z", shift(k)) for k in (1, 2, 3)]
    blocks = project(c.reshape(1), mine, other, *vals)
    blocks = [blocks[0]] + [lax.ppermute(blocks[k], "z", shift(-k)) for k in (1, 2, 3)]
    out, residual, ffn = dispatch(
        z.reshape(1), target, *blocks, tokens, ffn_gain, devices, capacity
    )
    arrived = lax.all_to_all(
        out.reshape(devices, capacity * 16, 128), everyone, 0, 0, tiled=True
    )
    base = shared(residual, ffn, shared_gate, shared_up, shared_down)
    result = experts(arrived, expert_gate, expert_up, expert_down)
    returned = lax.all_to_all(result, everyone, 0, 0, tiled=True)
    mixed = combine(
        target, weight.reshape(-1), returned.reshape(devices * capacity, 16, 128), base
    )
    return (mixed, latent_new, rotary_new)


def solution(mesh):
    grid = Mesh(mesh.devices.reshape(4, 4, 4, 2), ("z", "y", "x", "c"))
    ep = ("z", "y", "x", "c")
    return jax.shard_map(
        shards,
        mesh=grid,
        in_specs=(
            P(ep, None),
            P(ep),
            P(ep, None, None),
            P(ep, None, None),
            P(ep, None),
            P(ep, None),
            P(),
            P(),
            P(),
            P(),
            P(),
            P(),
            P(),
            P(),
            P(),
            P(),
            P(None, ep),
            P(),
            P(ep, None, None),
            P(ep, None, None),
            P(ep, None, None),
            P(),
            P(),
            P(),
        ),
        out_specs=(P(ep, None), P(ep, None), P(ep, None)),
        check_vma=False,
    )
```

```python
import functools

import jax
import jax.numpy as jnp
from jax import lax
from jax.experimental import pallas as pl
from jax.experimental.pallas import tpu as pltpu
from jax.sharding import Mesh
from jax.sharding import PartitionSpec as P

EPSILON = 1e-06
THETA = 10000.0
ROUTED_SCALE = 2.5
f32 = jnp.float32
bf16 = jnp.bfloat16

NT = (((1,), (1,)), ((), ()))
NN = (((1,), (0,)), ((), ()))
SEQ_STEP = 4


def dot(a, b, dims=NN):
    return lax.dot_general(a, b, dims, preferred_element_type=f32)


def rms(values, gain):
    squares = jnp.mean(values * values, axis=-1, keepdims=True)
    return values * lax.rsqrt(squares + EPSILON) * gain[None, :]


def turn(tile, cosine, sine):
    lane = lax.broadcasted_iota(jnp.int32, tile.shape, 1)
    swapped = jnp.where(lane % 32 < 16, pltpu.roll(tile, 112, 1), pltpu.roll(tile, 16, 1))
    return tile * cosine + swapped * sine


def attend_kernel(
    lengths,
    tokens,
    cosine,
    sine,
    attn_gain,
    q_gain,
    l_gain,
    w_qd_hbm,
    w_ld_hbm,
    w_rk_hbm,
    w_qn_hbm,
    w_ka_hbm,
    w_qr_hbm,
    w_vu_hbm,
    latent_hbm,
    rotary_hbm,
    values,
    latent_new,
    rotary_new,
    w_qd,
    w_ld,
    w_rk,
    w_qn,
    w_ka,
    w_qr,
    w_vu,
    latent,
    rotary,
    q_lat,
    q_rot,
    o_lat,
    l_new,
    r_new,
    scores_a,
    scores_b,
    sides_a,
    sides_b,
    sems,
):
    rows = tokens.shape[0]
    heads = w_ka.shape[0]
    lat = w_qd.shape[1]
    cache = latent.shape[1]
    halves = range(lat // 128)
    groups = rows // SEQ_STEP
    span = SEQ_STEP * heads
    rate = (w_ka.shape[1] + w_rk.shape[0]) ** (-0.5) * 1.4426950408889634
    moves = [
        pltpu.make_async_copy(a, b, sems.at[i])
        for i, (a, b) in enumerate(
            (
                (w_qd_hbm, w_qd),
                (w_ld_hbm, w_ld),
                (w_rk_hbm, w_rk),
                (w_qn_hbm, w_qn),
                (w_ka_hbm, w_ka),
                (w_qr_hbm, w_qr),
                (w_vu_hbm, w_vu),
            )
        )
    ]

    def fetches(g):
        part = pl.ds(g * SEQ_STEP, SEQ_STEP)
        return (
            pltpu.make_async_copy(latent_hbm.at[part], latent.at[part], sems.at[7 + g]),
            pltpu.make_async_copy(rotary_hbm.at[part], rotary.at[part], sems.at[7 + groups + g]),
        )

    for move in moves[:6]:
        move.start()
    for g in range(groups):
        for fetch in fetches(g):
            fetch.start()
    moves[6].start()

    normed = rms(tokens[...].astype(f32), attn_gain[...].astype(f32)).astype(bf16)
    moves[0].wait()
    low = rms(dot(normed, w_qd[...]), q_gain[...].astype(f32)).astype(bf16)
    moves[1].wait()
    fresh = rms(dot(normed, w_ld[...]), l_gain[...].astype(f32)).astype(bf16)
    latent_new[...] = fresh
    l_new[...] = fresh.astype(f32)
    cos, sin = cosine[...], sine[...]
    moves[2].wait()
    w_four = jnp.concatenate([w_rk[...]] * 4, axis=0)
    turned = turn(dot(normed, w_four, NT), cos, sin).astype(bf16)
    rotary_new[...] = turned[:, :32]
    r_new[...] = turned.astype(f32)
    moves[3].wait()
    nope = dot(low, w_qn[...]).astype(bf16)
    moves[4].wait()
    for h in range(heads):
        part = dot(nope[:, h * 64 : h * 64 + 64], w_ka[h])
        for g in range(rows // SEQ_STEP):
            at = g * span + h * SEQ_STEP
            for c in halves:
                q_lat[c, at : at + SEQ_STEP, :] = part[
                    g * SEQ_STEP : (g + 1) * SEQ_STEP, c * 128 : c * 128 + 128
                ]
    moves[5].wait()
    rope = dot(low, w_qr[...])
    member = lax.broadcasted_iota(jnp.int32, (rows, 128), 0) % SEQ_STEP
    inside = member == lax.broadcasted_iota(jnp.int32, (rows, 128), 1) // 32
    for j in range(heads // 4):
        tile = turn(rope[:, j * 128 : j * 128 + 128], cos, sin)
        moved = [tile] + [pltpu.roll(tile, 32 * k, 1) for k in (1, 2, 3)]
        for q in range(4):
            row = moved[-q % 4]
            for m in (1, 2, 3):
                row = jnp.where(member == m, moved[(m - q) % 4], row)
            row = jnp.where(inside, row, 0.0)
            for g in range(rows // SEQ_STEP):
                at = g * span + (4 * j + q) * SEQ_STEP
                q_rot[at : at + SEQ_STEP, :] = row[g * SEQ_STEP : (g + 1) * SEQ_STEP]

    owner = lax.broadcasted_iota(jnp.int32, (span, lat), 0) % SEQ_STEP
    group = lax.broadcasted_iota(jnp.int32, (1, 128), 1) // 32
    lane = lax.broadcasted_iota(jnp.int32, (1, span), 1) % SEQ_STEP
    place = lax.broadcasted_iota(jnp.int32, (cache, span), 0)
    mine = lax.broadcasted_iota(jnp.int32, (span, cache), 0) % SEQ_STEP

    def score(g, scores_ref, sides_ref):
        first = g * SEQ_STEP
        base = pl.multiple_of(g * span, span)
        for fetch in fetches(g):
            fetch.wait()
        q_all = jnp.concatenate([q_lat[c, pl.ds(base, span), :] for c in halves], axis=1).astype(
            bf16
        )
        new_rot = jnp.zeros((1, 128), f32)
        limit = jnp.zeros((1, span), jnp.int32)
        news, queries = [], []
        for j in range(SEQ_STEP):
            new_rot = jnp.where(group == j, r_new[pl.ds(first + j, 1), :], new_rot)
            limit = jnp.where(lane == j, lengths[first + j], limit)
            news.append(l_new[pl.ds(first + j, 1), :])
            queries.append(jnp.where(owner == j, q_all, jnp.zeros_like(q_all)))
        fresh = jnp.broadcast_to(jnp.concatenate(news, axis=1), (16, SEQ_STEP * lat)).astype(bf16)
        keys = jnp.concatenate([latent[first + j] for j in range(SEQ_STEP)], axis=1)
        rot_q = q_rot[pl.ds(base, span), :].astype(bf16)
        rot_keys = rotary[pl.ds(first, SEQ_STEP)].reshape(SEQ_STEP * 32, cache)
        turned = dot(rot_q, rot_keys).T
        both = dot(
            jnp.concatenate([keys, fresh], axis=0), jnp.concatenate(queries, axis=1), NT
        )
        own = dot(jnp.broadcast_to(new_rot, (16, 128)).astype(bf16), rot_q, NT)
        own = ((both[cache:] + own) * rate)[:1]
        scores = jnp.where(place < limit, (both[:cache] + turned) * rate, -jnp.inf)
        scores_ref[...] = scores
        top = jnp.maximum(jnp.max(scores, axis=0, keepdims=True), own)
        sides_ref[0:1, :] = top
        sides_ref[1:2, :] = jnp.exp2(own - top)

    def gather(g, scores_ref, sides_ref):
        first = g * SEQ_STEP
        base = pl.multiple_of(g * span, span)
        weights = jnp.exp2(scores_ref[...] - sides_ref[0:1, :])
        own_weight = sides_ref[1:2, :]
        inverse = 1.0 / (jnp.sum(weights, axis=0, keepdims=True) + own_weight)
        pick = lax.broadcasted_iota(jnp.int32, (8, span), 0) == 0
        sides = jnp.where(pick, inverse, own_weight).T
        probs = weights.T.astype(bf16)
        out = None
        for j in range(SEQ_STEP):
            part = dot(jnp.where(mine == j, probs, jnp.zeros_like(probs)), latent[first + j])
            out = part if j == 0 else out + part
        new_rows = l_new[pl.ds(first, 1), :]
        for j in range(1, SEQ_STEP):
            new_rows = jnp.where(owner == j, l_new[pl.ds(first + j, 1), :], new_rows)
        out = (out + sides[:, 1:2] * new_rows) * sides[:, :1]
        for c in halves:
            o_lat[c, pl.ds(base, span), :] = out[:, c * 128 : c * 128 + 128]

    score(0, scores_a, sides_a)

    def pair_of_groups(i, carry):
        g = 2 * i
        score(g + 1, scores_b, sides_b)
        gather(g, scores_a, sides_a)
        score(g + 2, scores_a, sides_a)
        gather(g + 1, scores_b, sides_b)
        return carry

    lax.fori_loop(0, groups // 2 - 1, pair_of_groups, 0)
    score(groups - 1, scores_b, sides_b)
    gather(groups - 2, scores_a, sides_a)
    gather(groups - 1, scores_b, sides_b)

    moves[6].wait()
    for p in range(heads // 2):
        pair = []
        for h in (2 * p, 2 * p + 1):
            parts = []
            for g in range(rows // SEQ_STEP):
                at = g * span + h * SEQ_STEP
                parts.append(
                    jnp.concatenate([o_lat[c, at : at + SEQ_STEP, :] for c in halves], axis=1)
                )
            pair.append(dot(jnp.concatenate(parts, axis=0).astype(bf16), w_vu[h], NT))
        values[:, p * 128 : p * 128 + 128] = jnp.concatenate(pair, axis=1).astype(bf16)


def whole(shape):
    zeros = (0,) * len(shape)
    return pl.BlockSpec(shape, lambda *_: zeros)


def smem():
    return pl.BlockSpec(memory_space=pltpu.SMEM)


def vmem():
    return pl.BlockSpec(memory_space=pltpu.VMEM)


def room(mib):
    return pltpu.CompilerParams(vmem_limit_bytes=mib * 2**20)


def far_away(array):
    return pltpu.with_memory_space_constraint(array, pltpu.HBM)


def near_core(*arrays):
    return [pltpu.with_memory_space_constraint(a, pltpu.VMEM) for a in arrays]


def attend(small, large):
    rows, model = small[1].shape
    lat, rope = large[0].shape[1], large[2].shape[0]
    heads = large[4].shape[0]
    far = pl.BlockSpec(memory_space=pl.ANY)
    groups = rows // SEQ_STEP
    return pl.pallas_call(
        attend_kernel,
        grid=(1,),
        in_specs=[smem()] + [whole(a.shape) for a in small[1:]] + [far] * len(large),
        out_specs=[vmem(), whole((rows, lat)), whole((rows, rope))],
        out_shape=[
            pltpu.VMEM((rows, model), bf16),
            jax.ShapeDtypeStruct((rows, lat), bf16),
            jax.ShapeDtypeStruct((rows, rope), bf16),
        ],
        scratch_shapes=[
            *[pltpu.VMEM(a.shape, bf16) for a in large],
            pltpu.VMEM((lat // 128, rows * heads, 128), f32),
            pltpu.VMEM((rows * heads, 128), f32),
            pltpu.VMEM((lat // 128, rows * heads, 128), f32),
            pltpu.VMEM((rows, lat), f32),
            pltpu.VMEM((rows, 128), f32),
            pltpu.VMEM((large[7].shape[1], SEQ_STEP * heads), f32),
            pltpu.VMEM((large[7].shape[1], SEQ_STEP * heads), f32),
            pltpu.VMEM((8, SEQ_STEP * heads), f32),
            pltpu.VMEM((8, SEQ_STEP * heads), f32),
            pltpu.SemaphoreType.DMA((7 + 2 * groups,)),
        ],
        cost_estimate=pl.CostEstimate(
            flops=4 * 10**9, bytes_accessed=22 * 10**6, transcendentals=10**6
        ),
        compiler_params=room(40),
        name="attend",
    )(*small, *[far_away(a) for a in large])


def copies_kernel(columns, out):
    for k in range(out.shape[0]):
        out[k] = columns[...]


def copies(columns, count):
    return pl.pallas_call(
        copies_kernel,
        in_specs=[vmem()],
        out_specs=vmem(),
        out_shape=pltpu.VMEM((count,) + columns.shape, bf16),
        compiler_params=room(4),
        name="copies",
    )(*near_core(columns))


def project_kernel(side, mine, other, v0, v1, v2, v3, o0, o1, o2, o3, w):
    c = side[0]
    w[:, c] = mine[...]
    w[:, 1 - c] = other[...]
    rows = v0.shape[0]
    vals = jnp.concatenate([v0[...], v1[...], v2[...], v3[...]], axis=0)
    columns = w[...].reshape(w.shape[0] * 2 * w.shape[2], w.shape[3])
    result = dot(vals, columns, NT).astype(bf16)
    for k, out in enumerate((o0, o1, o2, o3)):
        out[...] = result[k * rows : (k + 1) * rows]


def project(side, mine, other, *vals):
    groups, cols, model = mine.shape
    shape = (vals[0].shape[0], groups * 2 * cols)
    return pl.pallas_call(
        project_kernel,
        in_specs=[smem()] + [vmem()] * 6,
        out_specs=[vmem()] * 4,
        out_shape=[pltpu.VMEM(shape, bf16)] * 4,
        scratch_shapes=[
            pltpu.VMEM((groups, 2, cols, model), bf16),
        ],
        compiler_params=room(12),
        name="project",
    )(side, *near_core(mine, other), *near_core(*vals))


def dispatch_kernel(
    place, target, h0, h1, h2, h3, tokens, gain, out, residual, ffn, blocks, tiles
):
    z = place[0]
    rows = tokens.shape[0]
    for k, block in enumerate((h0, h1, h2, h3)):
        blocks[(z + k) % 4] = block[...]
    attended = jnp.concatenate([blocks[b] for b in range(4)], axis=1)
    total = (tokens[...].astype(f32) + attended.astype(f32)).astype(bf16)
    residual[...] = total
    normed = rms(total.astype(f32), gain[...].astype(f32))
    ffn[...] = normed.astype(bf16)
    for c in range(16):
        tiles[pl.ds(c, rows, stride=16), :] = normed[:, c * 128 : c * 128 + 128]
    out[...] = jnp.zeros_like(out)

    def send(t, carry):
        tile = tiles[pl.ds(pl.multiple_of(t * 16, 16), 16), :].astype(bf16)
        for k in range(6):
            out[target[t * 6 + k]] = tile
        return carry

    lax.fori_loop(0, rows, send, 0, unroll=4)


def dispatch(place, target, h0, h1, h2, h3, tokens, gain, devices, capacity):
    rows, model = tokens.shape
    return pl.pallas_call(
        dispatch_kernel,
        in_specs=[smem(), smem()] + [vmem()] * 6,
        out_specs=[vmem()] * 3,
        out_shape=[
            pltpu.VMEM((devices * capacity, 16, 128), bf16),
            pltpu.VMEM((rows, model), bf16),
            pltpu.VMEM((rows, model), bf16),
        ],
        scratch_shapes=[
            pltpu.VMEM((4, rows, model // 4), bf16),
            pltpu.VMEM((rows * 16, 128), f32),
        ],
        compiler_params=room(10),
        name="dispatch",
    )(place, target, *near_core(h0, h1, h2, h3, tokens, gain))


def shared_kernel(residual, ffn, gate, up, down, out):
    g = dot(ffn[...], gate[...])
    hidden = (g * jax.nn.sigmoid(g) * dot(ffn[...], up[...])).astype(bf16)
    out[...] = residual[...].astype(f32) + dot(hidden, down[...])


def shared(residual, ffn, gate, up, down):
    args = (residual, ffn, gate, up, down)
    return pl.pallas_call(
        shared_kernel,
        in_specs=[vmem()] * 5,
        out_specs=vmem(),
        out_shape=pltpu.VMEM(residual.shape, f32),
        cost_estimate=pl.CostEstimate(
            flops=10**9, bytes_accessed=4 * 10**6, transcendentals=10**4
        ),
        compiler_params=room(10),
        name="shared",
    )(*near_core(*args))


def expert_kernel(arrived, gate, up, down, out, wide, x, w_gate, w_up, w_down, sems):
    peers, depth, lanes = arrived.shape
    slots = depth // 16
    moves = [
        pltpu.make_async_copy(a.at[0], b, sems.at[i])
        for i, (a, b) in enumerate(((gate, w_gate), (up, w_up), (down, w_down)))
    ]
    for move in moves:
        move.start()
    wide[...] = arrived[...].astype(f32).reshape(peers * depth, lanes)
    for s in range(slots):
        for c in range(16):
            rows = wide[pl.ds(s * 16 + c, peers, stride=depth), :]
            x[s * peers : (s + 1) * peers, c * 128 : c * 128 + 128] = rows.astype(bf16)
    moves[0].wait()
    g = dot(x[...], w_gate[...])
    moves[1].wait()
    hidden = (g * jax.nn.sigmoid(g) * dot(x[...], w_up[...])).astype(bf16)
    moves[2].wait()
    result = dot(hidden, w_down[...])
    for s in range(slots):
        for c in range(16):
            wide[pl.ds(s * 16 + c, peers, stride=depth), :] = result[
                s * peers : (s + 1) * peers, c * 128 : c * 128 + 128
            ]
    out[...] = wide[...].reshape(peers, depth, lanes).astype(bf16)


def experts(arrived, gate, up, down):
    peers, depth, lanes = arrived.shape
    return pl.pallas_call(
        expert_kernel,
        in_specs=[vmem()] + [pl.BlockSpec(memory_space=pl.ANY)] * 3,
        out_specs=vmem(),
        out_shape=pltpu.VMEM(arrived.shape, bf16),
        scratch_shapes=[
            pltpu.VMEM((peers * depth, lanes), f32),
            pltpu.VMEM((peers * depth // 16, 2048), bf16),
            *[pltpu.VMEM(w.shape[1:], bf16) for w in (gate, up, down)],
            pltpu.SemaphoreType.DMA((3,)),
        ],
        compiler_params=room(24),
        name="experts",
    )(*near_core(arrived), *[far_away(w) for w in (gate, up, down)])


def combine_kernel(target, weight, returned, base, out, tiles):
    rows = base.shape[0]

    def gather(t, carry):
        total = jnp.zeros((16, 128), f32)
        for k in range(6):
            p = t * 6 + k
            total = total + returned[target[p]].astype(f32) * weight[p]
        tiles[pl.ds(pl.multiple_of(t * 16, 16), 16), :] = total
        return carry

    lax.fori_loop(0, rows, gather, 0, unroll=4)
    for c in range(16):
        sl = slice(c * 128, c * 128 + 128)
        out[:, sl] = (base[:, sl] + tiles[pl.ds(c, rows, stride=16), :]).astype(bf16)


def combine(target, weight, returned, base):
    rows = base.shape[0]
    return pl.pallas_call(
        combine_kernel,
        in_specs=[smem(), smem(), vmem(), vmem()],
        out_specs=vmem(),
        out_shape=pltpu.VMEM(base.shape, bf16),
        scratch_shapes=[pltpu.VMEM((rows * 16, 128), f32)],
        compiler_params=room(8),
        name="combine",
    )(target, weight, *near_core(returned, base))


def shards(
    tokens,
    lengths,
    latent_cache,
    rotary_cache,
    route_ids,
    route_scores,
    attn_gain,
    w_query_down,
    query_gain,
    w_query_nope,
    w_query_rope,
    w_key_absorb,
    latent_gain,
    w_latent_down,
    w_rotary_key,
    w_value_up,
    w_output,
    ffn_gain,
    expert_gate,
    expert_up,
    expert_down,
    shared_gate,
    shared_up,
    shared_down,
):
    rows, model = tokens.shape
    rotary = w_rotary_key.shape[1]
    top = route_ids.shape[1]
    devices = 128
    capacity = 3
    everyone = ("z", "y", "x", "c")
    z, c = lax.axis_index("z"), lax.axis_index("c")

    columns = w_output.T
    sent = copies(columns, 16)
    mine = lax.all_to_all(sent, ("y", "x"), 0, 0, tiled=True)

    half = rotary // 2
    freqs = 1.0 / THETA ** (jnp.arange(half, dtype=f32) * 2.0 / rotary)
    angles = lengths.astype(f32)[:, None] * jnp.tile(freqs, 8)[None, :]
    sign = jnp.where(jnp.arange(128) % rotary < half, -1.0, 1.0)
    cosine, sine = jnp.cos(angles), jnp.sin(angles) * sign[None, :]

    values, latent_new, rotary_new = attend(
        (lengths, tokens, cosine, sine, attn_gain, query_gain, latent_gain),
        (
            w_query_down,
            w_latent_down,
            w_rotary_key.T,
            w_query_nope,
            w_key_absorb,
            w_query_rope,
            w_value_up.transpose(0, 2, 1),
            latent_cache,
            rotary_cache.transpose(0, 2, 1),
        ),
    )

    same = route_ids[:, None, :, None] == route_ids[None, :, None, :]
    before = jnp.arange(rows)[None, :] < jnp.arange(rows)[:, None]
    slot = jnp.sum((same & before[:, :, None, None]).astype(jnp.int32), axis=(1, 3))
    target = (route_ids * capacity + slot).reshape(-1)
    weight = ROUTED_SCALE * route_scores / jnp.sum(route_scores, axis=1, keepdims=True)

    mine, values = lax.optimization_barrier((mine, values))
    other = lax.ppermute(mine, "c", [(0, 1), (1, 0)])
    def shift(k):
        return [(i, (i + k) % 4) for i in range(4)]

    vals = [values] + [lax.ppermute(values, "z", shift(k)) for k in (1, 2, 3)]
    blocks = project(c.reshape(1), mine, other, *vals)
    blocks = [blocks[0]] + [lax.ppermute(blocks[k], "z", shift(-k)) for k in (1, 2, 3)]
    out, residual, ffn = dispatch(
        z.reshape(1), target, *blocks, tokens, ffn_gain, devices, capacity
    )
    arrived = lax.all_to_all(
        out.reshape(devices, capacity * 16, 128), everyone, 0, 0, tiled=True
    )
    base = shared(residual, ffn, shared_gate, shared_up, shared_down)
    result = experts(arrived, expert_gate, expert_up, expert_down)
    returned = lax.all_to_all(result, everyone, 0, 0, tiled=True)
    mixed = combine(
        target, weight.reshape(-1), returned.reshape(devices * capacity, 16, 128), base
    )
    return (mixed, latent_new, rotary_new)


def solution(mesh):
    grid = Mesh(mesh.devices.reshape(4, 4, 4, 2), ("z", "y", "x", "c"))
    ep = ("z", "y", "x", "c")
    return jax.shard_map(
        shards,
        mesh=grid,
        in_specs=(
            P(ep, None),
            P(ep),
            P(ep, None, None),
            P(ep, None, None),
            P(ep, None),
            P(ep, None),
            P(),
            P(),
            P(),
            P(),
            P(),
            P(),
            P(),
            P(),
            P(),
            P(),
            P(None, ep),
            P(),
            P(ep, None, None),
            P(ep, None, None),
            P(ep, None, None),
            P(),
            P(),
            P(),
        ),
        out_specs=(P(ep, None), P(ep, None), P(ep, None)),
        check_vma=False,
    )
```
